32 devices in a mesh: sp: 8 (over z, y), tp: 4 (over x, core).
Axes of the slice: x: 2, y: 2, z: 4, core: 2. Of those that a mesh axis runs over, the one named last changes fastest.
Arguments:
- residual_in: bfloat16 [3072, 2048], P(('sp', 'tp')), may hold values from -6 to 6
- queries: bfloat16 [3072, 2048], P('sp', 'tp'), may hold values from -180 to 180
- keys: bfloat16 [3072, 2048], P('sp', 'tp'), may hold values from -9 to 9
- values: bfloat16 [3072, 2048], P('sp', 'tp'), may hold values from -6 to 6
- mix_lambda: float32 [16], P('tp'), may hold values from 0.3 to 0.8
- head_gain: float32 [128], replicated, may hold values from 0.1 to 1.9
- out_weight: bfloat16 [2048, 2048], P('tp'), may hold values from -0.125 to 0.125
- norm_gain: float32 [2048], replicated, may hold values from 0.1 to 1.9
- gate_weight: bfloat16 [2048, 5632], P('sp', 'tp'), may hold values from -0.125 to 0.125
- up_weight: bfloat16 [2048, 5632], P('sp', 'tp'), may hold values from -0.125 to 0.125
- down_weight: bfloat16 [5632, 2048], P('tp', 'sp'), may hold values from -0.078125 to 0.078125
Outputs:
- layer_out: bfloat16 [3072, 2048], P(('sp', 'tp'))
The draws below stay inside these ranges and needn't reach their ends.
All inputs are finite; a program needn't handle non-finite values.
Results may differ from the reference program's by a relative error of at most 0.014.
Values may be sent and summed in bfloat16 or wider, within the bound.
A program may use at most 128 MiB of HBM per device.

```python
import math
import jax
import jax.numpy as jnp
from jax import lax

D = 2048
H = 16
DH = 64
VD = 128
FF = 5632
TOKENS = 3072


def shared_keys(key):
    base = jax.random.fold_in(key, 101)
    drawn = jnp.clip(1.3 * jax.random.normal(jax.random.fold_in(base, 1), (TOKENS, H * 2 * DH), jnp.float32), -8.0, 8.0)
    return drawn


def draw_keys(key, part):
    drawn = shared_keys(key)
    return drawn.astype(jnp.bfloat16)


def draw_queries(key, part):
    base = jax.random.fold_in(key, 202)
    drawn = jnp.clip(1.3 * jax.random.normal(jax.random.fold_in(base, 1), (TOKENS, H * 2 * DH), jnp.float32), -8.0, 8.0)
    return drawn.astype(jnp.bfloat16)


def block_levels(own_key, dims, shards, low, largest):
    loudness, own = 1.0, jax.random.fold_in(own_key, 6)
    for position, parts in shards:
        heights = jnp.exp(jax.random.uniform(jax.random.fold_in(own, position), (parts,), jnp.float32, low / len(shards), largest / len(shards)))
        loudness = loudness * jnp.repeat(heights, dims[position] // parts).reshape([-1 if axis == position else 1 for axis in range(len(dims))])
    return loudness


def bell_draw(key, extent, width, limit, cuts=(), kind=jnp.bfloat16):
    values = jax.random.normal(key, extent, jnp.float32) * width
    if len(cuts) > 0:
        values = block_levels(key, extent, cuts, -0.22, 0.18) * values
    return jnp.clip(values, min=-limit, max=limit).astype(kind)


def setup_inputs(seed: int = 0) -> dict:
    arg_keys = jax.random.split(jax.random.key(seed), 12)
    return {
        "residual_in": bell_draw(arg_keys[0], (TOKENS, D), 1.0, 6.0, ((0, 32),)),
        "queries": draw_queries(jax.random.fold_in(arg_keys[11], 71), 0),
        "keys": draw_keys(jax.random.fold_in(arg_keys[11], 71), 0),
        "values": bell_draw(arg_keys[3], (TOKENS, H * VD), 1.0, 6.0, ((0, 8), (1, 4))),
        "mix_lambda": jnp.clip(0.3 + 0.5 * jax.random.uniform(arg_keys[4], (H,), jnp.float32) ** block_levels(arg_keys[4], (H,), ((0, 4),), -0.2, 0.2), 0.3, 0.8),
        "head_gain": jnp.clip(1.0 + 0.18 * jax.random.normal(arg_keys[5], (VD,), jnp.float32), 0.1, 1.9),
        "out_weight": bell_draw(arg_keys[6], (H * VD, D), (H * VD) ** -0.5, 0.125, ((0, 4),)),
        "norm_gain": jnp.clip(1.0 + 0.18 * jax.random.normal(arg_keys[7], (D,), jnp.float32), 0.1, 1.9),
        "gate_weight": bell_draw(arg_keys[8], (D, FF), D ** -0.5, 0.125, ((0, 8), (1, 4))),
        "up_weight": bell_draw(arg_keys[9], (D, FF), D ** -0.5, 0.125, ((0, 8), (1, 4))),
        "down_weight": bell_draw(arg_keys[10], (FF, D), FF ** -0.5, 0.078125, ((0, 4), (1, 8))),
    }


def head_rows(args):
    query_head, key_head, value_head, weight_two, head_gain = args
    block_rows = math.gcd(512, TOKENS)
    blocks = query_head.reshape(TOKENS // block_rows, block_rows, 2, DH)
    key_float = key_head.astype(jnp.float32)
    value_float = value_head.astype(jnp.float32)

    def one_block(query_block):
        scores = jnp.einsum('qcd,kcd->cqk', query_block.astype(jnp.float32), key_float) / math.sqrt(DH)
        top = lax.optimization_barrier(jnp.max(scores, axis=-1, keepdims=True))
        expo = jnp.exp(scores - top)
        total = lax.optimization_barrier(jnp.sum(expo, axis=-1, keepdims=True))
        probs = lax.optimization_barrier(expo.astype(jnp.bfloat16)).astype(jnp.float32)
        maps = jnp.einsum('cqk,ke->cqe', probs, value_float) / total
        mixed = maps[0] - weight_two * maps[1]
        scale = lax.rsqrt(lax.optimization_barrier(jnp.mean(mixed * mixed, axis=-1, keepdims=True)) + 1e-06)
        return (mixed * scale * head_gain).astype(jnp.bfloat16)
    return lax.map(one_block, blocks).reshape(TOKENS, VD)

def reference(residual_in, queries, keys, values, mix_lambda, head_gain, out_weight, norm_gain, gate_weight, up_weight, down_weight):
    query_heads = jnp.transpose(queries.reshape(TOKENS, H, 2, DH), (1, 0, 2, 3))
    key_heads = jnp.transpose(keys.reshape(TOKENS, H, 2, DH), (1, 0, 2, 3))
    value_heads = jnp.transpose(values.reshape(TOKENS, H, VD), (1, 0, 2))
    gains = jnp.broadcast_to(head_gain, (H, VD))
    per_head = lax.map(head_rows, (query_heads, key_heads, value_heads, mix_lambda, gains))
    attended = jnp.transpose(per_head, (1, 0, 2)).reshape(TOKENS, H * VD)
    after_mix = residual_in.astype(jnp.float32) + jnp.dot(attended, out_weight, preferred_element_type=jnp.float32)
    scale = lax.rsqrt(lax.optimization_barrier(jnp.mean(after_mix * after_mix, axis=-1, keepdims=True)) + 1e-06)
    normed = (after_mix * scale * norm_gain).astype(jnp.bfloat16)
    gate = jnp.dot(normed, gate_weight, preferred_element_type=jnp.float32)
    up = jnp.dot(normed, up_weight, preferred_element_type=jnp.float32)
    hidden = (jax.nn.silu(gate) * up).astype(jnp.bfloat16)
    mixer = jnp.dot(hidden, down_weight, preferred_element_type=jnp.float32)
    return (after_mix + 0.5 * mixer).astype(jnp.bfloat16)
```

```python
import functools
import math

import jax
import jax.numpy as jnp
from jax import lax
from jax.experimental import pallas as pl
from jax.experimental.pallas import tpu as pltpu
from jax.sharding import Mesh, PartitionSpec as P

DH = 64
VD = 128
LOG2E = 1.4426950408889634


def attention_kernel(heads, lam_ref, gain_ref, q_ref, k_ref, v_ref, o_ref, vx_ref):
    @pl.when(pl.program_id(0) == 0)
    def _():
        for h in range(heads):
            vx_ref[:, 2 * h * VD : (2 * h + 1) * VD] = v_ref[:, h * VD : (h + 1) * VD]
            vx_ref[:, (2 * h + 1) * VD : (2 * h + 2) * VD] = jnp.ones(
                (v_ref.shape[0], VD), jnp.bfloat16
            )

    scale = LOG2E / math.sqrt(DH)
    for h in range(heads):
        cols = slice(h * VD, (h + 1) * VD)
        q = q_ref[:, cols]
        lane = lax.broadcasted_iota(jnp.int32, q.shape, 1)
        maps = []
        for c in range(2):
            qc = jnp.where((lane >= DH) if c else (lane < DH), q, jnp.zeros_like(q))
            s = lax.dot_general(
                qc, k_ref[:, cols], (((1,), (1,)), ((), ())), preferred_element_type=jnp.float32
            )
            top = jnp.max(s, axis=-1, keepdims=True)
            e = jnp.exp2((s - top) * scale).astype(jnp.bfloat16)
            w = jnp.dot(
                e, vx_ref[:, 2 * h * VD : (2 * h + 2) * VD], preferred_element_type=jnp.float32
            )
            maps.append(w[:, :VD] / w[:, VD:])
        mixed = maps[0] - lam_ref[0:1, cols] * maps[1]
        norm = lax.rsqrt(jnp.mean(mixed * mixed, axis=-1, keepdims=True) + 1e-06)
        o_ref[:, cols] = (mixed * norm * gain_ref[...]).astype(jnp.bfloat16)


def attention(q, k, v, lam, gain):
    rows, width = q.shape
    heads = width // VD
    block = math.gcd(rows, 256)
    lam_wide = jnp.repeat(lam, VD).reshape(1, width)
    return pl.pallas_call(
        functools.partial(attention_kernel, heads),
        grid=(rows // block,),
        out_shape=jax.ShapeDtypeStruct((rows, width), jnp.bfloat16),
        in_specs=[
            pl.BlockSpec((1, width), lambda i: (0, 0)),
            pl.BlockSpec((1, VD), lambda i: (0, 0)),
            pl.BlockSpec((block, width), lambda i: (i, 0)),
            pl.BlockSpec(k.shape, lambda i: (0, 0)),
            pl.BlockSpec(v.shape, lambda i: (0, 0)),
        ],
        out_specs=pl.BlockSpec((block, width), lambda i: (i, 0)),
        scratch_shapes=[pltpu.VMEM((v.shape[0], 2 * width), jnp.bfloat16)],
        compiler_params=pltpu.CompilerParams(vmem_limit_bytes=60 * 1024 * 1024),
        cost_estimate=pl.CostEstimate(
            flops=rows * k.shape[0] * width * 8, bytes_accessed=4 * k.size * 2, transcendentals=0
        ),
    )(lam_wide, gain.reshape(1, VD), q, k, v)


def body(
    residual_in,
    queries,
    keys,
    values,
    mix_lambda,
    head_gain,
    out_weight,
    norm_gain,
    gate_weight,
    up_weight,
    down_weight,
):
    za, yb, tp = (lax.axis_size(name) for name in ("za", "yb", "tp"))
    tok_local, width = queries.shape
    rows, model = residual_in.shape
    heads = mix_lambda.shape[0] // za
    own = width // za

    def to_heads(a):
        return lax.all_to_all(a.reshape(tok_local, za, own), "za", 1, 0, tiled=False)

    qkv = jnp.stack(
        [a.reshape(tok_local, za, own).transpose(1, 0, 2) for a in (queries, keys, values)], 1
    )
    qkv = lax.all_to_all(qkv, "za", 0, 0, tiled=True)
    q = qkv[:, 0].reshape(za * tok_local, own)
    kv = lax.all_gather(qkv[:, 1:].transpose(1, 0, 2, 3), "yb", axis=1, tiled=True)
    k, v = kv[0].reshape(-1, own), kv[1].reshape(-1, own)

    lam = lax.dynamic_slice_in_dim(mix_lambda, lax.axis_index("za") * heads, heads, 0)
    out = attention(q, k, v, lam, head_gain)
    out = lax.all_to_all(
        out.reshape(za * tp, rows, own), ("za", "tp"), 0, 0, tiled=True
    )
    attended = (
        out.reshape(za, tp, rows, own).transpose(2, 1, 0, 3).reshape(rows, tp * width)
    )

    weights = jnp.stack([gate_weight.T, up_weight.T, down_weight])
    hid, depth = weights.shape[1] // za, weights.shape[2]
    weights = weights.reshape(3, za, hid, depth).transpose(1, 0, 2, 3)
    weights = lax.all_to_all(weights, "za", 0, 0, tiled=True)
    weights = lax.all_gather(weights, "yb", axis=0, tiled=False)
    weights = weights.transpose(2, 3, 1, 0, 4).reshape(3, hid, model)

    out_full = lax.all_gather(out_weight, "tp", axis=0, tiled=True)
    after = residual_in.astype(jnp.float32) + jnp.dot(
        attended, out_full, preferred_element_type=jnp.float32
    )
    row_scale = lax.rsqrt(jnp.mean(after * after, axis=-1, keepdims=True) + 1e-06)
    normed = (after * row_scale * norm_gain).astype(jnp.bfloat16)
    all_rows = lax.all_gather(normed, ("za", "tp"), axis=0, tiled=True)
    contract = (((1,), (1,)), ((), ()))
    gate = lax.dot_general(all_rows, weights[0], contract, preferred_element_type=jnp.float32)
    up = lax.dot_general(all_rows, weights[1], contract, preferred_element_type=jnp.float32)
    hidden = (jax.nn.silu(gate) * up).astype(jnp.bfloat16)
    mixer = lax.psum_scatter(
        jnp.dot(hidden, weights[2], preferred_element_type=jnp.float32).astype(jnp.bfloat16),
        ("za", "tp"),
        scatter_dimension=0,
        tiled=True,
    ).astype(jnp.float32)
    return (after + 0.5 * mixer).astype(jnp.bfloat16)


def solution(mesh):
    sp, tp = mesh.shape["sp"], mesh.shape["tp"]

    def run(*args):
        heads_local = args[4].shape[0] // tp
        za = math.gcd(heads_local, sp)
        cut = Mesh(mesh.devices.reshape(za, sp // za, tp), ("za", "yb", "tp"))
        s = ("za", "yb")
        return jax.shard_map(
            body,
            mesh=cut,
            in_specs=(
                P(("za", "yb", "tp"), None),
                P(s, "tp"),
                P(s, "tp"),
                P(s, "tp"),
                P("tp"),
                P(),
                P("tp", None),
                P(),
                P(s, "tp"),
                P(s, "tp"),
                P("tp", s),
            ),
            out_specs=P(("za", "yb", "tp"), None),
            check_vma=False,
        )(*args)

    return run
```

```python
import functools
import math

import jax
import jax.numpy as jnp
from jax import lax
from jax.experimental import pallas as pl
from jax.experimental.pallas import tpu as pltpu
from jax.sharding import Mesh, PartitionSpec as P

DH = 64
VD = 128
LOG2E = 1.4426950408889634


MESH = pl.DeviceIdType.MESH
AXES = ("za", "yb", "tp")


def remote(src, dst, send, recv, **where):
    return pltpu.make_async_remote_copy(
        src_ref=src, dst_ref=dst, send_sem=send, recv_sem=recv, device_id=where, device_id_type=MESH
    )


def front_kernel(n, lam_ref, gain_ref, qkv, w, o_out, w_out, scr, kk, vx, osend,
                 q_s, q_r, y_s, y_r, w_s, w_r, wy_s, wy_r, o_s, o_r, l_s):
    nz, ny, nt, heads, aligned = n
    z, y, t = (lax.axis_index(name) for name in AXES)
    tok, rows = scr.shape[3], osend.shape[1]
    depth = w.shape[2]

    def place(zz, yy):
        at = zz * ny + yy
        return w_out.at[:, pl.ds(pl.multiple_of(at * depth, depth), depth)] if aligned else w_out.at[at]

    barrier = pltpu.get_barrier_semaphore()
    me = z * nt + t
    for i in range(1, nz * nt):
        p = lax.rem(me + i, nz * nt)
        pl.semaphore_signal(barrier, inc=1, device_id={"za": p // nt, "tp": lax.rem(p, nt)}, device_id_type=MESH)
    for f in range(1, ny):
        pl.semaphore_signal(barrier, inc=1, device_id={"yb": lax.rem(y + f, ny)}, device_id_type=MESH)
    pl.semaphore_wait(barrier, nz * nt - 1 + ny - 1)

    def q_copy(d):
        zp = lax.rem(z + d, nz)
        return remote(qkv.at[zp], scr.at[z, y], q_s.at[d], q_r.at[z], za=zp)

    def kv_own(f):
        return remote(qkv.at[z, pl.ds(1, 2)], scr.at[z, y, pl.ds(1, 2)], y_s.at[0, f], y_r.at[z, y],
                      yb=lax.rem(y + f, ny))

    def kv_copy(d, f):
        zp = lax.rem(z + d, nz)
        part = scr.at[zp, y, pl.ds(1, 2)]
        return remote(part, part, y_s.at[d, f], y_r.at[zp, y], yb=lax.rem(y + f, ny))

    def w_copy(d):
        zp = lax.rem(z + d, nz)
        return remote(w.at[zp], place(z, y), w_s.at[d], w_r.at[z], za=zp)

    def w_own(f):
        return remote(w.at[z], place(z, y), wy_s.at[0, f], wy_r.at[z, y], yb=lax.rem(y + f, ny))

    def w_pass(d, f):
        zp = lax.rem(z + d, nz)
        return remote(place(zp, y), place(zp, y), wy_s.at[d, f], wy_r.at[zp, y], yb=lax.rem(y + f, ny))

    for d in range(1, nz):
        q_copy(d).start()
    for f in range(1, ny):
        kv_own(f).start()
    local = pltpu.make_async_copy(w.at[z], place(z, y), l_s)
    local.start()
    for d in range(1, nz):
        w_copy(d).start()
    for f in range(1, ny):
        w_own(f).start()
    scr[z, y] = qkv[z]
    for d in range(1, nz):
        zp = lax.rem(z + d, nz)
        remote(qkv.at[z], scr.at[zp, y], q_s.at[d], q_r.at[zp], za=zp).wait_recv()
        for f in range(1, ny):
            kv_copy(d, f).start()
    for d in range(nz):
        zp = lax.rem(z + d, nz)
        for f in range(1, ny):
            yp = lax.rem(y + f, ny)
            part = scr.at[zp, yp, pl.ds(1, 2)]
            remote(part, part, y_s.at[d, f], y_r.at[zp, yp], yb=yp).wait_recv()
    for zz in range(nz):
        for yy in range(ny):
            span = slice((zz * ny + yy) * tok, (zz * ny + yy + 1) * tok)
            kk[span] = scr[zz, yy, 1]
            for h in range(heads):
                vx[span, 2 * h * VD : (2 * h + 1) * VD] = scr[zz, yy, 2, :, h * VD : (h + 1) * VD]
                vx[span, (2 * h + 1) * VD : (2 * h + 2) * VD] = jnp.ones((tok, VD), jnp.bfloat16)

    scale = LOG2E / math.sqrt(DH)

    def o_copy(p):
        return remote(osend.at[p], o_out.at[me], o_s.at[p], o_r.at[me], za=p // nt, tp=lax.rem(p, nt))

    def block(i, carry):
        zq = i // (nt // 2)
        off = lax.rem(i, nt // 2) * (2 * rows)
        for h in range(heads):
            cols = slice(h * VD, (h + 1) * VD)
            q = scr[zq, y, 0, pl.ds(pl.multiple_of(off, 2 * rows), 2 * rows), cols]
            lane = lax.broadcasted_iota(jnp.int32, q.shape, 1)
            maps = []
            for c in range(2):
                qc = jnp.where((lane >= DH) if c else (lane < DH), q, jnp.zeros_like(q))
                s = lax.dot_general(
                    qc, kk[:, cols], (((1,), (1,)), ((), ())), preferred_element_type=jnp.float32
                )
                top = jnp.max(s, axis=-1, keepdims=True)
                e = jnp.exp2((s - top) * scale).astype(jnp.bfloat16)
                o = jnp.dot(
                    e, vx[:, 2 * h * VD : (2 * h + 2) * VD], preferred_element_type=jnp.float32
                )
                maps.append(o[:, :VD] / o[:, VD:])
            mixed = maps[0] - lam_ref[0:1, cols] * maps[1]
            norm = lax.rsqrt(jnp.mean(mixed * mixed, axis=-1, keepdims=True) + 1e-06)
            done = (mixed * norm * gain_ref[...]).astype(jnp.bfloat16)
            osend[2 * i, :, cols] = done[:rows]
            osend[2 * i + 1, :, cols] = done[rows:]
        for j in range(2):
            p = 2 * i + j

            @pl.when(p != me)
            def _():
                o_copy(p).start()

        return carry

    lax.fori_loop(0, nz * nt // 2, block, 0)
    o_out[me] = osend[me]
    for d in range(1, nz):
        zp = lax.rem(z + d, nz)
        remote(w.at[z], place(zp, y), w_s.at[d], w_r.at[zp], za=zp).wait_recv()
        if d == 1:
            local.wait()
        for f in range(1, ny):
            w_pass(d, f).start()
    for i in range(1, nz * nt):
        p = lax.rem(me + i, nz * nt)
        remote(osend.at[p], o_out.at[p], o_s.at[p], o_r.at[p], za=p // nt, tp=lax.rem(p, nt)).wait_recv()
        o_copy(p).wait_send()
    for d in range(nz):
        zp = lax.rem(z + d, nz)
        for f in range(1, ny):
            yp = lax.rem(y + f, ny)
            remote(place(zp, yp), place(zp, yp), wy_s.at[d, f], wy_r.at[zp, yp], yb=yp).wait_recv()
            if d:
                w_pass(d, f).wait_send()
                kv_copy(d, f).wait_send()
            else:
                w_own(f).wait_send()
                kv_own(f).wait_send()
        if d:
            q_copy(d).wait_send()
            w_copy(d).wait_send()


def front(qkv, weights, lam, gain, rows, sizes):
    nz, ny, nt, heads = sizes
    tok, own = qkv.shape[2:]
    hid, depth = weights.shape[1:]
    aligned = depth % 128 == 0
    w_shape = (hid, nz * ny * depth) if aligned else (nz * ny, hid, depth)
    vmem = pl.BlockSpec(memory_space=pltpu.VMEM)
    dma = pltpu.SemaphoreType.DMA
    out, gathered = pl.pallas_call(
        functools.partial(front_kernel, (nz, ny, nt, heads, aligned)),
        out_shape=(
            jax.ShapeDtypeStruct((nz * nt, rows, own), jnp.bfloat16),
            jax.ShapeDtypeStruct(w_shape, jnp.bfloat16),
        ),
        in_specs=[vmem, vmem, vmem, pl.BlockSpec(memory_space=pl.ANY)],
        out_specs=(vmem, pl.BlockSpec(memory_space=pl.ANY)),
        scratch_shapes=[
            pltpu.VMEM((nz, ny, 3, tok, own), jnp.bfloat16),
            pltpu.VMEM((nz * ny * tok, own), jnp.bfloat16),
            pltpu.VMEM((nz * ny * tok, 2 * own), jnp.bfloat16),
            pltpu.VMEM((nz * nt, rows, own), jnp.bfloat16),
            dma((nz,)), dma((nz,)),
            dma((nz, ny)), dma((nz, ny)),
            dma((nz,)), dma((nz,)),
            dma((nz, ny)), dma((nz, ny)),
            dma((nz * nt,)), dma((nz * nt,)),
            dma,
        ],
        compiler_params=pltpu.CompilerParams(
            collective_id=1, has_side_effects=True, vmem_limit_bytes=60 * 1024 * 1024
        ),
        cost_estimate=pl.CostEstimate(
            flops=100_000_000_000, bytes_accessed=20_000_000, transcendentals=0
        ),
    )(jnp.repeat(lam, VD).reshape(1, own), gain.reshape(1, VD), qkv, weights)
    if not aligned:
        gathered = gathered.transpose(1, 0, 2).reshape(hid, nz * ny * depth)
    return out, gathered


def mixer_kernel(n, normed, after, w, out, got, mine, c_send, c_recv, x_send, x_recv, z_send, z_recv,
                 az_s, az_r, ax_s, ax_r, ac_s, ac_r, rc_s, rc_r, rx_s, rx_r, rz_s, rz_r):
    nz, nx = n
    z, y, t = (lax.axis_index(name) for name in AXES)
    x, c = t // 2, lax.rem(t, 2)
    other = 1 - c
    rows, model = normed.shape
    hid = w.shape[0] // 3

    barrier = pltpu.get_barrier_semaphore()
    for d in range(1, nz):
        pl.semaphore_signal(barrier, inc=1, device_id={"za": lax.rem(z + d, nz)}, device_id_type=MESH)
    for e in range(1, nx):
        pl.semaphore_signal(barrier, inc=1, device_id={"tp": lax.rem(x + e, nx) * 2 + c}, device_id_type=MESH)
    pl.semaphore_signal(barrier, inc=1, device_id={"tp": x * 2 + other}, device_id_type=MESH)
    pl.semaphore_wait(barrier, nz + nx - 1)

    def at(d, e):
        return lax.rem(z + d, nz), lax.rem(x + e, nx)

    def slot(d, e, cc):
        zp, xp = at(d, e)
        return got.at[zp, xp, pl.ds(pl.multiple_of(cc * rows, rows), rows)]

    def ag_z(d):
        return remote(normed, slot(0, 0, c), az_s.at[d], az_r.at[z], za=lax.rem(z + d, nz))

    def ag_x(d, e):
        src = slot(d, 0, c) if d else normed
        return remote(src, slot(d, 0, c), ax_s.at[d, e], ax_r.at[lax.rem(z + d, nz), x],
                      tp=lax.rem(x + e, nx) * 2 + c)

    def ag_c(d, e):
        zp, xp = at(d, e)
        src = slot(d, e, c) if (d or e) else normed
        return remote(src, slot(d, e, c), ac_s.at[d, e], ac_r.at[zp, xp], tp=x * 2 + other)

    def rs_c(d, e):
        return remote(c_send.at[d, e], c_recv.at[d, e], rc_s.at[d, e], rc_r.at[d, e], tp=x * 2 + other)

    def rs_x(d, e):
        return remote(x_send.at[d, e], x_recv.at[d, e], rx_s.at[d, e], rx_r.at[d, e],
                      tp=lax.rem(x + e, nx) * 2 + c)

    def rs_z(d):
        return remote(z_send.at[d], z_recv.at[d], rz_s.at[d], rz_r.at[d], za=lax.rem(z + d, nz))

    for d in range(1, nz):
        ag_z(d).start()
    for e in range(1, nx):
        ag_x(0, e).start()
    ag_c(0, 0).start()
    got[z, x, pl.ds(pl.multiple_of(c * rows, rows), rows)] = normed[...]

    def after_core(d, e):
        rs_c(d, e).wait_recv()
        both = mine[d, e].astype(jnp.float32) + c_recv[d, e].astype(jnp.float32)
        if e:
            x_send[d, e] = both.astype(jnp.bfloat16)
            rs_x(d, e).start()
        else:
            mine[d, e] = both

    def after_x(d):
        total = mine[d, 0]
        for e in range(1, nx):
            rs_x(d, e).wait_recv()
            total = total + x_recv[d, e].astype(jnp.float32)
        if d:
            z_send[d] = total.astype(jnp.bfloat16)
            rs_z(d).start()
        else:
            mine[0, 0] = total

    steps = [(d, e) for d in range(nz) for e in range(nx)]
    contract = (((1,), (1,)), ((), ()))
    for k, (d, e) in enumerate(steps):
        zp, xp = at(d, e)
        if d and e == 0:
            remote(normed, slot(d, 0, c), az_s.at[d], az_r.at[zp], za=zp).wait_recv()
            for f in range(1, nx):
                ag_x(d, f).start()
            ag_c(d, 0).start()
        if e:
            remote(normed, slot(d, e, c), ax_s.at[d, e], ax_r.at[zp, xp], tp=xp * 2 + c).wait_recv()
            ag_c(d, e).start()
        remote(normed, slot(d, e, other), ac_s.at[d, e], ac_r.at[zp, xp], tp=x * 2 + other).wait_recv()
        block = got[zp, xp]
        gate = lax.dot_general(block, w[0:hid], contract, preferred_element_type=jnp.float32)
        up = lax.dot_general(block, w[hid : 2 * hid], contract, preferred_element_type=jnp.float32)
        hidden = (jax.nn.silu(gate) * up).astype(jnp.bfloat16)
        part = jnp.dot(hidden, w[2 * hid :], preferred_element_type=jnp.float32)
        low, high = part[:rows], part[rows:]
        mine[d, e] = jnp.where(c == 0, low, high)
        c_send[d, e] = jnp.where(c == 0, high, low).astype(jnp.bfloat16)
        rs_c(d, e).start()
        if k:
            after_core(*steps[k - 1])
        if d and e == nx - 1:
            after_x(d - 1)
    after_core(*steps[-1])
    after_x(nz - 1)
    total = mine[0, 0]
    for d in range(1, nz):
        rs_z(d).wait_recv()
        total = total + z_recv[d].astype(jnp.float32)
    out[...] = (after[...] + 0.5 * total).astype(jnp.bfloat16)
    for d, e in steps:
        ag_c(d, e).wait_send()
        rs_c(d, e).wait_send()
        if e:
            ag_x(d, e).wait_send()
            rs_x(d, e).wait_send()
        elif d:
            ag_z(d).wait_send()
            rs_z(d).wait_send()


def mixer_call(normed, after, weights, sizes):
    nz, nx = sizes
    rows, model = normed.shape
    dma = pltpu.SemaphoreType.DMA
    vmem = pl.BlockSpec(memory_space=pltpu.VMEM)
    half = (nz, nx, rows, model)
    return pl.pallas_call(
        functools.partial(mixer_kernel, sizes),
        out_shape=jax.ShapeDtypeStruct((rows, model), jnp.bfloat16),
        in_specs=[vmem] * 3,
        out_specs=vmem,
        scratch_shapes=[
            pltpu.VMEM((nz, nx, 2 * rows, model), jnp.bfloat16),
            pltpu.VMEM(half, jnp.float32),
            pltpu.VMEM(half, jnp.bfloat16),
            pltpu.VMEM(half, jnp.bfloat16),
            pltpu.VMEM(half, jnp.bfloat16),
            pltpu.VMEM(half, jnp.bfloat16),
            pltpu.VMEM((nz, rows, model), jnp.bfloat16),
            pltpu.VMEM((nz, rows, model), jnp.bfloat16),
            dma((nz,)), dma((nz,)),
            dma((nz, nx)), dma((nz, nx)),
            dma((nz, nx)), dma((nz, nx)),
            dma((nz, nx)), dma((nz, nx)),
            dma((nz, nx)), dma((nz, nx)),
            dma((nz,)), dma((nz,)),
        ],
        compiler_params=pltpu.CompilerParams(
            collective_id=2, has_side_effects=True, vmem_limit_bytes=62 * 1024 * 1024
        ),
        cost_estimate=pl.CostEstimate(
            flops=100_000_000_000, bytes_accessed=20_000_000, transcendentals=0
        ),
    )(normed, after, weights)


def body(
    residual_in,
    queries,
    keys,
    values,
    mix_lambda,
    head_gain,
    out_weight,
    norm_gain,
    gate_weight,
    up_weight,
    down_weight,
):
    za, yb, tp = (lax.axis_size(name) for name in AXES)
    tok_local, width = queries.shape
    rows, model = residual_in.shape
    heads = mix_lambda.shape[0] // za
    own = width // za

    out_full = lax.all_gather(out_weight, "tp", axis=0, tiled=True)
    qkv = jnp.stack(
        [a.reshape(tok_local, za, own).transpose(1, 0, 2) for a in (queries, keys, values)], 1
    )
    hid = down_weight.shape[0] // za
    weights = jnp.stack(
        [a.reshape(za, hid, -1) for a in (gate_weight.T, up_weight.T, down_weight)], 1
    ).reshape(za, 3 * hid, -1)
    lam = lax.dynamic_slice_in_dim(mix_lambda, lax.axis_index("za") * heads, heads, 0)
    out, weights = front(qkv, weights, lam, head_gain, rows, (za, yb, tp, heads))
    attended = (
        out.reshape(za, tp, rows, own).transpose(2, 1, 0, 3).reshape(rows, tp * width)
    )
    after = residual_in.astype(jnp.float32) + jnp.dot(
        attended, out_full, preferred_element_type=jnp.float32
    )
    row_scale = lax.rsqrt(jnp.mean(after * after, axis=-1, keepdims=True) + 1e-06)
    normed = (after * row_scale * norm_gain).astype(jnp.bfloat16)
    return mixer_call(normed, after, weights, (za, tp // 2))


def solution(mesh):
    sp, tp = mesh.shape["sp"], mesh.shape["tp"]

    def run(*args):
        heads_local = args[4].shape[0] // tp
        za = math.gcd(heads_local, sp)
        cut = Mesh(mesh.devices.reshape(za, sp // za, tp), ("za", "yb", "tp"))
        s = ("za", "yb")
        return jax.shard_map(
            body,
            mesh=cut,
            in_specs=(
                P(("za", "yb", "tp"), None),
                P(s, "tp"),
                P(s, "tp"),
                P(s, "tp"),
                P("tp"),
                P(),
                P("tp", None),
                P(),
                P(s, "tp"),
                P(s, "tp"),
                P("tp", s),
            ),
            out_specs=P(("za", "yb", "tp"), None),
            check_vma=False,
        )(*args)

    return run
```

```python
import functools
import math

import jax
import jax.numpy as jnp
from jax import lax
from jax.experimental import pallas as pl
from jax.experimental.pallas import tpu as pltpu
from jax.sharding import Mesh, PartitionSpec as P

DH = 64
VD = 128
LOG2E = 1.4426950408889634


MESH = pl.DeviceIdType.MESH
AXES = ("za", "yb", "tp")


def remote(src, dst, send, recv, **where):
    return pltpu.make_async_remote_copy(
        src_ref=src, dst_ref=dst, send_sem=send, recv_sem=recv, device_id=where, device_id_type=MESH
    )


def front_kernel(n, lam_ref, gain_ref, qkv, w, o_out, w_out, scr, kk, vx, osend,
                 q_s, q_r, y_s, y_r, w_s, w_r, wy_s, wy_r, o_s, o_r, l_s):
    nz, ny, nt, heads, aligned = n
    z, y, t = (lax.axis_index(name) for name in AXES)
    tok, rows = scr.shape[3], osend.shape[1]
    depth = w.shape[2]

    def place(zz, yy):
        at = zz * ny + yy
        return w_out.at[:, pl.ds(pl.multiple_of(at * depth, depth), depth)] if aligned else w_out.at[at]

    barrier = pltpu.get_barrier_semaphore()
    me = z * nt + t
    for i in range(1, nz * nt):
        p = lax.rem(me + i, nz * nt)
        pl.semaphore_signal(barrier, inc=1, device_id={"za": p // nt, "tp": lax.rem(p, nt)}, device_id_type=MESH)
    for f in range(1, ny):
        pl.semaphore_signal(barrier, inc=1, device_id={"yb": lax.rem(y + f, ny)}, device_id_type=MESH)
    pl.semaphore_wait(barrier, nz * nt - 1 + ny - 1)

    def q_copy(d):
        zp = lax.rem(z + d, nz)
        return remote(qkv.at[zp], scr.at[z, y], q_s.at[d], q_r.at[z], za=zp)

    def kv_own(f):
        return remote(qkv.at[z, pl.ds(1, 2)], scr.at[z, y, pl.ds(1, 2)], y_s.at[0, f], y_r.at[z, y],
                      yb=lax.rem(y + f, ny))

    def kv_copy(d, f):
        zp = lax.rem(z + d, nz)
        part = scr.at[zp, y, pl.ds(1, 2)]
        return remote(part, part, y_s.at[d, f], y_r.at[zp, y], yb=lax.rem(y + f, ny))

    def w_copy(d):
        zp = lax.rem(z + d, nz)
        return remote(w.at[zp], place(z, y), w_s.at[d], w_r.at[z], za=zp)

    def w_own(f):
        return remote(w.at[z], place(z, y), wy_s.at[0, f], wy_r.at[z, y], yb=lax.rem(y + f, ny))

    def w_pass(d, f):
        zp = lax.rem(z + d, nz)
        return remote(place(zp, y), place(zp, y), wy_s.at[d, f], wy_r.at[zp, y], yb=lax.rem(y + f, ny))

    for d in range(nz - 1, 0, -1):
        q_copy(d).start()
    for f in range(1, ny):
        kv_own(f).start()
    local = pltpu.make_async_copy(w.at[z], place(z, y), l_s)
    local.start()
    for d in range(nz - 1, 0, -1):
        w_copy(d).start()
    for f in range(1, ny):
        w_own(f).start()
    scr[z, y] = qkv[z]
    for d in range(1, nz):
        zp = lax.rem(z + d, nz)
        remote(qkv.at[z], scr.at[zp, y], q_s.at[d], q_r.at[zp], za=zp).wait_recv()
        for f in range(1, ny):
            kv_copy(d, f).start()
    for d in range(nz):
        zp = lax.rem(z + d, nz)
        for f in range(1, ny):
            yp = lax.rem(y + f, ny)
            part = scr.at[zp, yp, pl.ds(1, 2)]
            remote(part, part, y_s.at[d, f], y_r.at[zp, yp], yb=yp).wait_recv()
    for zz in range(nz):
        for yy in range(ny):
            span = slice((zz * ny + yy) * tok, (zz * ny + yy + 1) * tok)
            kk[span] = scr[zz, yy, 1]
            for h in range(heads):
                vx[span, 2 * h * VD : (2 * h + 1) * VD] = scr[zz, yy, 2, :, h * VD : (h + 1) * VD]
                vx[span, (2 * h + 1) * VD : (2 * h + 2) * VD] = jnp.ones((tok, VD), jnp.bfloat16)

    scale = LOG2E / math.sqrt(DH)

    def o_copy(p):
        return remote(osend.at[p], o_out.at[me], o_s.at[p], o_r.at[me], za=p // nt, tp=lax.rem(p, nt))

    def block(i, carry):
        zq = i // (nt // 2)
        off = lax.rem(i, nt // 2) * (2 * rows)
        for h in range(heads):
            cols = slice(h * VD, (h + 1) * VD)
            q = scr[zq, y, 0, pl.ds(pl.multiple_of(off, 2 * rows), 2 * rows), cols]
            lane = lax.broadcasted_iota(jnp.int32, q.shape, 1)
            maps = []
            for c in range(2):
                qc = jnp.where((lane >= DH) if c else (lane < DH), q, jnp.zeros_like(q))
                s = lax.dot_general(
                    qc, kk[:, cols], (((1,), (1,)), ((), ())), preferred_element_type=jnp.float32
                )
                top = jnp.max(s, axis=-1, keepdims=True)
                e = jnp.exp2((s - top) * scale).astype(jnp.bfloat16)
                o = jnp.dot(
                    e, vx[:, 2 * h * VD : (2 * h + 2) * VD], preferred_element_type=jnp.float32
                )
                maps.append(o[:, :VD] / o[:, VD:])
            mixed = maps[0] - lam_ref[0:1, cols] * maps[1]
            norm = lax.rsqrt(jnp.mean(mixed * mixed, axis=-1, keepdims=True) + 1e-06)
            done = (mixed * norm * gain_ref[...]).astype(jnp.bfloat16)
            osend[2 * i, :, cols] = done[:rows]
            osend[2 * i + 1, :, cols] = done[rows:]
        for j in range(2):
            p = 2 * i + j

            @pl.when(p != me)
            def _():
                o_copy(p).start()

        @pl.when(i == nz * nt // 2 - 2)
        def _():
            w_take(1)

        return carry

    def w_take(d):
        zp = lax.rem(z + d, nz)
        remote(w.at[z], place(zp, y), w_s.at[d], w_r.at[zp], za=zp).wait_recv()
        for f in range(1, ny):
            w_pass(d, f).start()

    lax.fori_loop(0, nz * nt // 2, block, 0)
    o_out[me] = osend[me]
    local.wait()
    for d in range(2, nz):
        w_take(d)
    for i in range(1, nz * nt):
        p = lax.rem(me + i, nz * nt)
        remote(osend.at[p], o_out.at[p], o_s.at[p], o_r.at[p], za=p // nt, tp=lax.rem(p, nt)).wait_recv()
        o_copy(p).wait_send()
    for d in range(nz):
        zp = lax.rem(z + d, nz)
        for f in range(1, ny):
            yp = lax.rem(y + f, ny)
            remote(place(zp, yp), place(zp, yp), wy_s.at[d, f], wy_r.at[zp, yp], yb=yp).wait_recv()
            if d:
                w_pass(d, f).wait_send()
                kv_copy(d, f).wait_send()
            else:
                w_own(f).wait_send()
                kv_own(f).wait_send()
        if d:
            q_copy(d).wait_send()
            w_copy(d).wait_send()


def front(qkv, weights, lam, gain, rows, sizes):
    nz, ny, nt, heads = sizes
    tok, own = qkv.shape[2:]
    hid, depth = weights.shape[1:]
    aligned = depth % 128 == 0
    w_shape = (hid, nz * ny * depth) if aligned else (nz * ny, hid, depth)
    vmem = pl.BlockSpec(memory_space=pltpu.VMEM)
    dma = pltpu.SemaphoreType.DMA
    out, gathered = pl.pallas_call(
        functools.partial(front_kernel, (nz, ny, nt, heads, aligned)),
        out_shape=(
            jax.ShapeDtypeStruct((nz * nt, rows, own), jnp.bfloat16),
            jax.ShapeDtypeStruct(w_shape, jnp.bfloat16),
        ),
        in_specs=[vmem, vmem, vmem, pl.BlockSpec(memory_space=pl.ANY)],
        out_specs=(vmem, pl.BlockSpec(memory_space=pl.ANY)),
        scratch_shapes=[
            pltpu.VMEM((nz, ny, 3, tok, own), jnp.bfloat16),
            pltpu.VMEM((nz * ny * tok, own), jnp.bfloat16),
            pltpu.VMEM((nz * ny * tok, 2 * own), jnp.bfloat16),
            pltpu.VMEM((nz * nt, rows, own), jnp.bfloat16),
            dma((nz,)), dma((nz,)),
            dma((nz, ny)), dma((nz, ny)),
            dma((nz,)), dma((nz,)),
            dma((nz, ny)), dma((nz, ny)),
            dma((nz * nt,)), dma((nz * nt,)),
            dma,
        ],
        compiler_params=pltpu.CompilerParams(
            collective_id=1, has_side_effects=True, vmem_limit_bytes=60 * 1024 * 1024
        ),
        cost_estimate=pl.CostEstimate(
            flops=100_000_000_000, bytes_accessed=20_000_000, transcendentals=0
        ),
    )(jnp.repeat(lam, VD).reshape(1, own), gain.reshape(1, VD), qkv, weights)
    if not aligned:
        gathered = gathered.transpose(1, 0, 2).reshape(hid, nz * ny * depth)
    return out, gathered


def mixer_kernel(n, normed, after, w, out, got, mine, c_send, c_recv, x_send, x_recv, z_send, z_recv,
                 az_s, az_r, ax_s, ax_r, ac_s, ac_r, rc_s, rc_r, rx_s, rx_r, rz_s, rz_r):
    nz, nx = n
    z, y, t = (lax.axis_index(name) for name in AXES)
    x, c = t // 2, lax.rem(t, 2)
    other = 1 - c
    rows, model = normed.shape
    hid = w.shape[0] // 3

    barrier = pltpu.get_barrier_semaphore()
    for d in range(1, nz):
        pl.semaphore_signal(barrier, inc=1, device_id={"za": lax.rem(z + d, nz)}, device_id_type=MESH)
    for e in range(1, nx):
        pl.semaphore_signal(barrier, inc=1, device_id={"tp": lax.rem(x + e, nx) * 2 + c}, device_id_type=MESH)
    pl.semaphore_signal(barrier, inc=1, device_id={"tp": x * 2 + other}, device_id_type=MESH)
    pl.semaphore_wait(barrier, nz + nx - 1)

    def at(d, e):
        return lax.rem(z + d, nz), lax.rem(x + e, nx)

    def slot(d, e, cc):
        zp, xp = at(d, e)
        return got.at[zp, xp, pl.ds(pl.multiple_of(cc * rows, rows), rows)]

    def ag_z(d):
        return remote(normed, slot(0, 0, c), az_s.at[d], az_r.at[z], za=lax.rem(z + d, nz))

    def ag_x(d, e):
        src = slot(d, 0, c) if d else normed
        return remote(src, slot(d, 0, c), ax_s.at[d, e], ax_r.at[lax.rem(z + d, nz), x],
                      tp=lax.rem(x + e, nx) * 2 + c)

    def ag_c(d, e):
        zp, xp = at(d, e)
        src = slot(d, e, c) if (d or e) else normed
        return remote(src, slot(d, e, c), ac_s.at[d, e], ac_r.at[zp, xp], tp=x * 2 + other)

    def rs_c(d, e):
        return remote(c_send.at[d, e], c_recv.at[d, e], rc_s.at[d, e], rc_r.at[d, e], tp=x * 2 + other)

    def rs_x(d, e):
        return remote(x_send.at[d, e], x_recv.at[d, e], rx_s.at[d, e], rx_r.at[d, e],
                      tp=lax.rem(x + e, nx) * 2 + c)

    def rs_z(d):
        return remote(z_send.at[d], z_recv.at[d], rz_s.at[d], rz_r.at[d], za=lax.rem(z + d, nz))

    for d in range(nz - 1, 0, -1):
        ag_z(d).start()
    for e in range(1, nx):
        ag_x(0, e).start()
    ag_c(0, 0).start()
    got[z, x, pl.ds(pl.multiple_of(c * rows, rows), rows)] = normed[...]

    def after_core(d, e):
        rs_c(d, e).wait_recv()
        both = mine[d, e].astype(jnp.float32) + c_recv[d, e].astype(jnp.float32)
        if e:
            x_send[d, e] = both.astype(jnp.bfloat16)
            rs_x(d, e).start()
        else:
            mine[d, e] = both

    def after_x(d):
        total = mine[d, 0]
        for e in range(1, nx):
            rs_x(d, e).wait_recv()
            total = total + x_recv[d, e].astype(jnp.float32)
        if d:
            z_send[d] = total.astype(jnp.bfloat16)
            rs_z(d).start()
        else:
            mine[0, 0] = total

    steps = [(d, e) for d in range(nz) for e in range(nx)]
    contract = (((1,), (1,)), ((), ()))
    for k, (d, e) in enumerate(steps):
        zp, xp = at(d, e)
        if d and e == 0:
            remote(normed, slot(d, 0, c), az_s.at[d], az_r.at[zp], za=zp).wait_recv()
            for f in range(1, nx):
                ag_x(d, f).start()
            ag_c(d, 0).start()
        if e:
            remote(normed, slot(d, e, c), ax_s.at[d, e], ax_r.at[zp, xp], tp=xp * 2 + c).wait_recv()
            ag_c(d, e).start()
        remote(normed, slot(d, e, other), ac_s.at[d, e], ac_r.at[zp, xp], tp=x * 2 + other).wait_recv()
        block = got[zp, xp]
        gate = lax.dot_general(block, w[0:hid], contract, preferred_element_type=jnp.float32)
        up = lax.dot_general(block, w[hid : 2 * hid], contract, preferred_element_type=jnp.float32)
        hidden = (jax.nn.silu(gate) * up).astype(jnp.bfloat16)
        part = jnp.dot(hidden, w[2 * hid :], preferred_element_type=jnp.float32)
        low, high = part[:rows], part[rows:]
        mine[d, e] = jnp.where(c == 0, low, high)
        c_send[d, e] = jnp.where(c == 0, high, low).astype(jnp.bfloat16)
        rs_c(d, e).start()
        if k:
            after_core(*steps[k - 1])
        if d and e == nx - 1:
            after_x(d - 1)
    after_core(*steps[-1])
    after_x(nz - 1)
    total = mine[0, 0]
    for d in range(1, nz):
        rs_z(d).wait_recv()
        total = total + z_recv[d].astype(jnp.float32)
    out[...] = (after[...] + 0.5 * total).astype(jnp.bfloat16)
    for d, e in steps:
        ag_c(d, e).wait_send()
        rs_c(d, e).wait_send()
        if e:
            ag_x(d, e).wait_send()
            rs_x(d, e).wait_send()
        elif d:
            ag_z(d).wait_send()
            rs_z(d).wait_send()


def mixer_call(normed, after, weights, sizes):
    nz, nx = sizes
    rows, model = normed.shape
    dma = pltpu.SemaphoreType.DMA
    vmem = pl.BlockSpec(memory_space=pltpu.VMEM)
    half = (nz, nx, rows, model)
    return pl.pallas_call(
        functools.partial(mixer_kernel, sizes),
        out_shape=jax.ShapeDtypeStruct((rows, model), jnp.bfloat16),
        in_specs=[vmem] * 3,
        out_specs=vmem,
        scratch_shapes=[
            pltpu.VMEM((nz, nx, 2 * rows, model), jnp.bfloat16),
            pltpu.VMEM(half, jnp.float32),
            pltpu.VMEM(half, jnp.bfloat16),
            pltpu.VMEM(half, jnp.bfloat16),
            pltpu.VMEM(half, jnp.bfloat16),
            pltpu.VMEM(half, jnp.bfloat16),
            pltpu.VMEM((nz, rows, model), jnp.bfloat16),
            pltpu.VMEM((nz, rows, model), jnp.bfloat16),
            dma((nz,)), dma((nz,)),
            dma((nz, nx)), dma((nz, nx)),
            dma((nz, nx)), dma((nz, nx)),
            dma((nz, nx)), dma((nz, nx)),
            dma((nz, nx)), dma((nz, nx)),
            dma((nz,)), dma((nz,)),
        ],
        compiler_params=pltpu.CompilerParams(
            collective_id=2, has_side_effects=True, vmem_limit_bytes=62 * 1024 * 1024
        ),
        cost_estimate=pl.CostEstimate(
            flops=100_000_000_000, bytes_accessed=20_000_000, transcendentals=0
        ),
    )(normed, after, weights)


def body(
    residual_in,
    queries,
    keys,
    values,
    mix_lambda,
    head_gain,
    out_weight,
    norm_gain,
    gate_weight,
    up_weight,
    down_weight,
):
    za, yb, tp = (lax.axis_size(name) for name in AXES)
    tok_local, width = queries.shape
    rows, model = residual_in.shape
    heads = mix_lambda.shape[0] // za
    own = width // za

    out_full = lax.all_gather(out_weight, "tp", axis=0, tiled=True)
    qkv = jnp.stack(
        [a.reshape(tok_local, za, own).transpose(1, 0, 2) for a in (queries, keys, values)], 1
    )
    hid = down_weight.shape[0] // za
    weights = jnp.stack(
        [a.reshape(za, hid, -1) for a in (gate_weight.T, up_weight.T, down_weight)], 1
    ).reshape(za, 3 * hid, -1)
    lam = lax.dynamic_slice_in_dim(mix_lambda, lax.axis_index("za") * heads, heads, 0)
    out, weights = front(qkv, weights, lam, head_gain, rows, (za, yb, tp, heads))
    attended = (
        out.reshape(za, tp, rows, own).transpose(2, 1, 0, 3).reshape(rows, tp * width)
    )
    after = residual_in.astype(jnp.float32) + jnp.dot(
        attended, out_full, preferred_element_type=jnp.float32
    )
    row_scale = lax.rsqrt(jnp.mean(after * after, axis=-1, keepdims=True) + 1e-06)
    normed = (after * row_scale * norm_gain).astype(jnp.bfloat16)
    return mixer_call(normed, after, weights, (za, tp // 2))


def solution(mesh):
    sp, tp = mesh.shape["sp"], mesh.shape["tp"]

    def run(*args):
        heads_local = args[4].shape[0] // tp
        za = math.gcd(heads_local, sp)
        cut = Mesh(mesh.devices.reshape(za, sp // za, tp), ("za", "yb", "tp"))
        s = ("za", "yb")
        return jax.shard_map(
            body,
            mesh=cut,
            in_specs=(
                P(("za", "yb", "tp"), None),
                P(s, "tp"),
                P(s, "tp"),
                P(s, "tp"),
                P("tp"),
                P(),
                P("tp", None),
                P(),
                P(s, "tp"),
                P(s, "tp"),
                P("tp", s),
            ),
            out_specs=P(("za", "yb", "tp"), None),
            check_vma=False,
        )(*args)

    return run
```
